32 devices in a mesh: tp: 8 (over z, x), dp: 4 (over y, core).
Axes of the slice: x: 2, y: 2, z: 4, core: 2. Of those that a mesh axis runs over, the one named last changes fastest.
Arguments:
- tokens: bfloat16 [128, 8, 4096], P('dp', None, 'tp'), may hold values from -12 to 12
- lengths: int32 [128], P('dp'), may hold values from 1 to 8, 384 in all
- norm_gains: float32 [2, 4096], replicated, may hold values from 0.1 to 1.9
- drive_proj: bfloat16 [2, 4096, 2048], P(None, 'dp', 'tp'), may hold values from -0.09375 to 0.09375
- open_proj: bfloat16 [2, 4096, 4096], P(None, 'dp', 'tp'), may hold values from -0.09375 to 0.09375
- glu_proj: bfloat16 [2, 2048, 2048], P(None, 'dp', 'tp'), may hold values from -0.125 to 0.125
- merge_proj: bfloat16 [2, 2048, 4096], P(None, 'dp', 'tp'), may hold values from -0.125 to 0.125
- exit_proj: bfloat16 [2, 4096, 4096], P(None, 'dp', 'tp'), may hold values from -0.09375 to 0.09375
- decay_rate: float32 [2, 128, 64], P(None, 'tp'), may hold values from 0.5 to 2
- turn_rate: float32 [2, 128, 64], P(None, 'tp'), may hold values from -3 to 3
- group_step_width: float32 [2, 128], P(None, 'tp'), may hold values from 0.005 to 0.3
- state_in: float32 [2, 2, 128, 64, 16], P(None, None, 'tp'), may hold values from -1 to 1
- state_out: float32 [2, 2, 128, 16, 64], P(None, None, 'tp'), may hold values from -0.5 to 0.5
- skip_gain: float32 [2, 2048], P(None, 'tp'), may hold values from -4 to 4
- carried_state: float32 [2, 2, 128, 8192], P(None, None, 'dp', 'tp'), may hold values from -6 to 6
Outputs:
- updated_tokens: bfloat16 [128, 8, 4096], P('dp', None, 'tp')
- new_state: float32 [2, 2, 128, 8192], P(None, None, 'dp', 'tp')
The draws below stay inside these ranges and needn't reach their ends.
Inputs may be any that keep to these rules, and one draw needn't show every extreme that they name: `lengths`: each sequence has at least one live slot, and some sequence has all 8.
All inputs are finite; a program needn't handle non-finite values. No bound on the sum of `lengths` on one device may be relied on, other than what follows from the above.
Results may differ from the reference program's by a relative error of at most 0.0055.
Values may be sent and summed in bfloat16 or wider, within the bound.
A program may use at most 128 MiB of HBM per device.

```python
import math
import jax
import jax.numpy as jnp
import numpy as np
from jax import lax

D = 4096
WIDTH = 2048
CHANNELS = 16
STATE = 64
STEPS = 8
LAYERS = 2
GROUPS = 128
BATCH = 128


def draw_tokens(key, part):
    first_key, second_key = jax.random.split(jax.random.fold_in(key, 11))
    block_count = 32
    blocks = jax.random.uniform(second_key, (BATCH, 1, block_count, 1), jnp.float32, math.log(0.3), math.log(3.0))
    factor = jnp.exp(blocks)
    values_drawn = jnp.clip(jax.random.normal(first_key, (BATCH, STEPS, block_count, D // block_count), jnp.float32), -4.0, 4.0)
    return (values_drawn * factor).reshape(BATCH, STEPS, D).astype(jnp.bfloat16)


def levels(key, shape, cuts, low, top_value):
    def one(dim, shards_of):
        heights = jax.random.uniform(jax.random.fold_in(jax.random.fold_in(key, 6), dim), (shards_of,), jnp.float32, low / len(cuts), top_value / len(cuts))
        return jnp.repeat(jnp.exp(heights), shape[dim] // shards_of).reshape((-1,) + (1,) * (len(shape) - dim - 1))

    gain = one(*cuts[0])
    for cut in cuts[1:]:
        gain = gain * one(*cut)
    return gain


def split_up(number_of, total, limit, slope):
    loads = [(1 << 20) // math.isqrt(grade ** slope) + 1 for grade in range(2, number_of + 1)]
    surplus, holding = total - limit - (number_of - 1), [1] * (number_of - 1)
    while surplus > 0:
        movable = [i for i in range(number_of - 1) if holding[i] < limit]
        pool, left = sum([loads[i] for i in movable]), surplus
        for i in movable:
            more = min(limit - holding[i], max(1, left * loads[i] // pool), surplus)
            holding[i] = holding[i] + more
            surplus = surplus - more
    return np.array([limit] + holding)


def uneven(stream_key, amount, total, reach, lean):
    if amount == 2:
        one = jax.random.randint(stream_key, (), max(1, total - reach), min(reach, total - 1) + 1)
        return jnp.stack([one, total - one])
    sizes = jnp.asarray(split_up(amount, total, reach, lean), jnp.int32)
    twos = (amount - 1) // 2
    donor, sink = sizes[1:1 + 2 * twos:2], sizes[2:2 + 2 * twos:2]
    room = jnp.minimum(donor - 1, reach - sink)
    passed = jax.random.randint(jax.random.fold_in(stream_key, 1), (twos,), 0, 1 << 20) % (room + 1)
    sizes = sizes.at[1:1 + 2 * twos:2].set(donor - passed).at[2:2 + 2 * twos:2].set(sink + passed)
    return sizes[jax.random.permutation(jax.random.fold_in(stream_key, 2), amount)]


def gaussian(stream_key, extent, scale, limit, cuts=(), dtype=jnp.bfloat16):
    loudness = levels(stream_key, extent, cuts, -0.22, 0.18) if cuts else 1.0
    array = jax.random.normal(stream_key, extent, jnp.float32) * scale * loudness
    return jnp.minimum(jnp.maximum(array, -limit), limit).astype(dtype)


def setup_inputs(seed: int = 0) -> dict:
    splits = jax.random.split(jax.random.key(seed), 16)
    return {
        "tokens": draw_tokens(jax.random.fold_in(splits[15], 71), 0),
        "lengths": uneven(splits[1], BATCH, 3 * BATCH, STEPS, 2).astype(jnp.int32),
        "norm_gains": jnp.clip(1.0 + 0.18 * jax.random.normal(splits[2], (LAYERS, D), jnp.float32), 0.1, 1.9),
        "drive_proj": gaussian(splits[3], (LAYERS, D, WIDTH), D ** -0.5, 0.09375, ((1, 4), (2, 8))),
        "open_proj": gaussian(splits[4], (LAYERS, D, D), D ** -0.5, 0.09375, ((1, 4), (2, 8))),
        "glu_proj": gaussian(splits[5], (LAYERS, WIDTH, WIDTH), WIDTH ** -0.5, 0.125, ((1, 4), (2, 8))),
        "merge_proj": gaussian(splits[6], (LAYERS, WIDTH, D), WIDTH ** -0.5, 0.125, ((1, 4), (2, 8))),
        "exit_proj": gaussian(splits[7], (LAYERS, D, D), D ** -0.5, 0.09375, ((1, 4), (2, 8))),
        "decay_rate": jnp.clip(jnp.exp(math.log(2.0) - 1.3862944 * jax.random.uniform(splits[8], (LAYERS, GROUPS, STATE), jnp.float32) ** levels(splits[8], (LAYERS, GROUPS, STATE), ((1, 8),), -0.2, 0.2)), 0.5, 2.0),
        "turn_rate": jnp.clip(jax.random.uniform(splits[9], (LAYERS, GROUPS, STATE), jnp.float32, -3.0, 3.0) * levels(splits[9], (LAYERS, GROUPS, STATE), ((1, 8),), -0.4, 0.0), -3.0, 3.0),
        "group_step_width": jnp.clip(jnp.exp(math.log(0.3) - 4.0943446 * jax.random.uniform(splits[10], (LAYERS, GROUPS), jnp.float32) ** levels(splits[10], (LAYERS, GROUPS), ((1, 8),), -0.2, 0.2)), 0.005, 0.3),
        "state_in": gaussian(splits[11], (LAYERS, 2, GROUPS, STATE, CHANNELS), (2 * CHANNELS) ** -0.5, 1.0, ((2, 8),), jnp.float32),
        "state_out": gaussian(splits[12], (LAYERS, 2, GROUPS, CHANNELS, STATE), (2 * STATE) ** -0.5, 0.5, ((2, 8),), jnp.float32),
        "skip_gain": gaussian(splits[13], (LAYERS, WIDTH), 1.0, 4.0, ((1, 8),), jnp.float32),
        "carried_state": gaussian(splits[14], (LAYERS, 2, BATCH, GROUPS * STATE), 1.0, 6.0, ((2, 4), (3, 8)), jnp.float32),
    }


EPS = 1e-05

def state_update(drive, active, current_rate, turn_now, size_now, in_pair, output_couple, skip_now, carried):
    sequences, positions = active.shape
    groups, entries = current_rate.shape
    members = in_pair.shape[-1]
    real_eig = -current_rate
    step_len = size_now[:, None]
    magnitude = jnp.exp(step_len * real_eig)
    decay_real = magnitude * jnp.cos(step_len * turn_now)
    decay_imag = magnitude * jnp.sin(step_len * turn_now)
    divisor = real_eig * real_eig + turn_now * turn_now
    hold_real = ((decay_real - 1.0) * real_eig + decay_imag * turn_now) / divisor
    hold_imag = (decay_imag * real_eig - (decay_real - 1.0) * turn_now) / divisor
    inject_real = hold_real[..., None] * in_pair[0] - hold_imag[..., None] * in_pair[1]
    inject_imag = hold_real[..., None] * in_pair[1] + hold_imag[..., None] * in_pair[0]
    inputs = drive.reshape(sequences, positions, groups, members)
    pushed_real = jnp.einsum('gpc,bsgc->bsgp', inject_real, inputs, precision=lax.Precision.HIGHEST)
    pushed_imag = jnp.einsum('gpc,bsgc->bsgp', inject_imag, inputs, precision=lax.Precision.HIGHEST)
    state_real_part = carried[0].reshape(sequences, groups, entries)
    state_imaginary = carried[1].reshape(sequences, groups, entries)
    readings = []
    for position in range(positions):
        active_now = (active[:, position] > 0)[:, None, None]
        moved_real = decay_real * state_real_part - decay_imag * state_imaginary + pushed_real[:, position]
        moved_imag = decay_real * state_imaginary + decay_imag * state_real_part + pushed_imag[:, position]
        state_real_part = jnp.where(active_now, moved_real, state_real_part)
        state_imaginary = jnp.where(active_now, moved_imag, state_imaginary)
        readout_value = jnp.einsum('sal,usl->usa', output_couple[0], state_real_part, precision=lax.Precision.HIGHEST) - jnp.einsum('sal,usl->usa', output_couple[1], state_imaginary, precision=lax.Precision.HIGHEST)
        readings.append(readout_value)
    readout = jnp.stack(readings, axis=1) + skip_now.reshape(groups, members) * inputs
    final = jnp.stack([state_real_part.reshape(sequences, groups * entries), state_imaginary.reshape(sequences, groups * entries)])
    return (readout.reshape(sequences * positions, groups * members), final)

def reference(tokens, lengths, norm_gains, drive_proj, open_proj, glu_proj, merge_proj, exit_proj, decay_rate, turn_rate, group_step_width, state_in, state_out, skip_gain, carried_state):
    sequences, positions, model_width = tokens.shape
    row_count = sequences * positions
    active = (lax.broadcasted_iota(jnp.int32, (sequences, positions), 1) < lengths[:, None]).astype(jnp.int32)
    active_rows = active.reshape(row_count, 1).astype(jnp.float32)
    residual = tokens.reshape(row_count, model_width)
    states = []
    for layer_index in range(LAYERS):
        values = residual.astype(jnp.float32)
        inverse_rms = lax.rsqrt(lax.optimization_barrier(jnp.mean(values * values, axis=1, keepdims=True)) + EPS)
        normed = (values * inverse_rms * norm_gains[layer_index]).astype(jnp.bfloat16)
        drive = jnp.dot(normed, drive_proj[layer_index], preferred_element_type=jnp.float32)
        gate_open = jax.nn.sigmoid(jnp.dot(normed, open_proj[layer_index], preferred_element_type=jnp.float32))
        readout, final = state_update(drive, active, decay_rate[layer_index], turn_rate[layer_index], group_step_width[layer_index], state_in[layer_index], state_out[layer_index], skip_gain[layer_index], carried_state[layer_index])
        states.append(final)
        activated = jax.nn.gelu(readout).astype(jnp.bfloat16)
        gating = jnp.dot(activated, glu_proj[layer_index], preferred_element_type=jnp.float32)
        gated = (activated.astype(jnp.float32) * jax.nn.sigmoid(gating)).astype(jnp.bfloat16)
        merged = jnp.dot(gated, merge_proj[layer_index], preferred_element_type=jnp.float32)
        mixed = (gate_open * merged).astype(jnp.bfloat16)
        branch = jnp.dot(mixed, exit_proj[layer_index], preferred_element_type=jnp.float32)
        residual = (residual.astype(jnp.float32) + active_rows * branch).astype(jnp.bfloat16)
    return (residual.reshape(sequences, positions, model_width), jnp.stack(states))
```

```python
import functools
import jax
import jax.numpy as jnp
from jax import lax
from jax.experimental import pallas as pl
from jax.experimental.pallas import tpu as pltpu
from jax.sharding import PartitionSpec as P

EPS = 1e-05


def state_update(
    drive, active, current_rate, turn_now, size_now, in_pair, output_couple, skip_now, carried
):
    sequences, positions = active.shape
    groups, entries = current_rate.shape
    members = in_pair.shape[-1]
    real_eig = -current_rate
    step_len = size_now[:, None]
    magnitude = jnp.exp(step_len * real_eig)
    decay_real = magnitude * jnp.cos(step_len * turn_now)
    decay_imag = magnitude * jnp.sin(step_len * turn_now)
    divisor = real_eig * real_eig + turn_now * turn_now
    hold_real = ((decay_real - 1.0) * real_eig + decay_imag * turn_now) / divisor
    hold_imag = (decay_imag * real_eig - (decay_real - 1.0) * turn_now) / divisor
    inject_real = hold_real[..., None] * in_pair[0] - hold_imag[..., None] * in_pair[1]
    inject_imag = hold_real[..., None] * in_pair[1] + hold_imag[..., None] * in_pair[0]
    inputs = drive.reshape(sequences, positions, groups, members)
    pushed_real = jnp.einsum("gpc,bsgc->bsgp", inject_real, inputs, precision=lax.Precision.HIGHEST)
    pushed_imag = jnp.einsum("gpc,bsgc->bsgp", inject_imag, inputs, precision=lax.Precision.HIGHEST)
    state_real_part = carried[0].reshape(sequences, groups, entries)
    state_imaginary = carried[1].reshape(sequences, groups, entries)
    readings = []
    for position in range(positions):
        active_now = (active[:, position] > 0)[:, None, None]
        moved_real = (
            decay_real * state_real_part - decay_imag * state_imaginary + pushed_real[:, position]
        )
        moved_imag = (
            decay_real * state_imaginary + decay_imag * state_real_part + pushed_imag[:, position]
        )
        state_real_part = jnp.where(active_now, moved_real, state_real_part)
        state_imaginary = jnp.where(active_now, moved_imag, state_imaginary)
        readout_value = jnp.einsum(
            "sal,usl->usa", output_couple[0], state_real_part, precision=lax.Precision.HIGHEST
        ) - jnp.einsum(
            "sal,usl->usa", output_couple[1], state_imaginary, precision=lax.Precision.HIGHEST
        )
        readings.append(readout_value)
    readout = jnp.stack(readings, axis=1) + skip_now.reshape(groups, members) * inputs
    final = jnp.stack(
        [
            state_real_part.reshape(sequences, groups * entries),
            state_imaginary.reshape(sequences, groups * entries),
        ]
    )
    return (readout.reshape(sequences * positions, groups * members), final)


def widen_model(values):
    return lax.all_gather(values, "tp", axis=1, tiled=True)


def widen_branch(values):
    return lax.all_gather(values, "tp", axis=1, tiled=True)


def project(gathered, weight):
    return jnp.dot(
        gathered,
        lax.all_gather(weight, "dp", axis=0, tiled=True),
        preferred_element_type=jnp.float32,
    )


def shards(
    tokens,
    lengths,
    norm_gains,
    drive_proj,
    open_proj,
    glu_proj,
    merge_proj,
    exit_proj,
    decay_rate,
    turn_rate,
    group_step_width,
    state_in,
    state_out,
    skip_gain,
    carried_state,
):
    sequences, positions, local_width = tokens.shape
    row_count = sequences * positions
    model_width = local_width * lax.axis_size("tp")
    first_col = lax.axis_index("tp") * local_width
    active = (lax.broadcasted_iota(jnp.int32, (sequences, positions), 1) < lengths[:, None]).astype(
        jnp.int32
    )
    active_rows = active.reshape(row_count, 1).astype(jnp.float32)
    residual = tokens.reshape(row_count, local_width)
    states = []
    for layer_index in range(norm_gains.shape[0]):
        norm_gain = norm_gains[layer_index]
        own_values = residual.astype(jnp.float32)
        squared_sum = lax.psum(jnp.sum(own_values * own_values, axis=1), "tp")
        inverse_rms = lax.rsqrt(squared_sum / model_width + EPS)[:, None]
        own_gain = lax.dynamic_slice_in_dim(norm_gain, first_col, local_width, 0)
        gathered = widen_model((own_values * inverse_rms * own_gain).astype(jnp.bfloat16))
        drive = project(gathered, drive_proj[layer_index])
        gate_open = jax.nn.sigmoid(project(gathered, open_proj[layer_index]))
        readout, final = state_update(
            drive,
            active,
            decay_rate[layer_index],
            turn_rate[layer_index],
            group_step_width[layer_index],
            state_in[layer_index],
            state_out[layer_index],
            skip_gain[layer_index],
            carried_state[layer_index],
        )
        states.append(final)
        activated = jax.nn.gelu(readout).astype(jnp.bfloat16)
        gating = project(widen_branch(activated), glu_proj[layer_index])
        gated = (activated.astype(jnp.float32) * jax.nn.sigmoid(gating)).astype(jnp.bfloat16)
        merged = project(widen_branch(gated), merge_proj[layer_index])
        mixed = (gate_open * merged).astype(jnp.bfloat16)
        branch = project(widen_model(mixed), exit_proj[layer_index])
        residual = (residual.astype(jnp.float32) + active_rows * branch).astype(jnp.bfloat16)
    return (residual.reshape(sequences, positions, local_width), jnp.stack(states))


LOTS = 3
SKEW = 0


def fused_kernel(
    dims,
    tok, lens, gains, rate, turn, size, s_in, s_out, skip, carried,
    w_drive, w_open, w_glu, w_merge, w_exit,
    out_tok, out_state,
    v_drive, v_open, v_glu, v_merge, v_exit, v_tok, v_in, v_out,
    par, inj, omx, len_own,
    row_send, row_recv, a_send, a_recv, c_send, c_recv,
    x_src, x_recv, y_src, y_recv, st_recv, st_new, fin_recv,
    norm_buf, inv_buf, act_buf, feed_buf, len_recv, pack_own, unpack,
    w_sem, in_sem, row_ss, row_rs, a_ss, a_rs, c_ss, c_rs, x_ss, x_rs, y_ss, y_rs,
    st_ss, st_rs, n_ss, n_rs, f_ss, f_rs, l_ss, l_rs,
):
    layers, nd, nt, all_rows, model, lots = dims
    ratio = nt // nd
    rows = all_rows // lots
    chunk = rows // nd
    half = rows // 2
    f32, bf16 = jnp.float32, jnp.bfloat16
    d = lax.axis_index("dp")
    t = lax.axis_index("tp")
    home = t // ratio
    place = lax.rem(t, ratio)
    batch_own = carried.shape[2]
    batch = batch_own * nd
    few, members, entries = v_in.shape[2:]
    own_ch = few * entries
    width = few * members
    own_rows = v_tok.shape[0]
    steps = own_rows // batch_own
    cols = v_tok.shape[1]

    def load(src, dst, sem):
        copy = pltpu.make_async_copy(src, dst, sem)
        copy.start()
        return copy

    tok_load = load(tok, v_tok, in_sem.at[0])
    in_load = load(s_in.at[:, :, pl.ds(d * few, few)], v_in, in_sem.at[1])
    out_load = load(s_out.at[:, :, pl.ds(d * few, few)], v_out, in_sem.at[2])

    barrier = pltpu.get_barrier_semaphore()
    total = nd * nt
    flat = t * nd + d

    def greet(i, carry):
        other = lax.rem(flat + i, total)
        pl.semaphore_signal(
            barrier, inc=1,
            device_id={"tp": other // nd, "dp": lax.rem(other, nd)},
            device_id_type=pl.DeviceIdType.MESH,
        )
        return carry

    lax.fori_loop(1, total, greet, 0)

    loads = {}
    for l in range(layers):
        for i, (src, dst) in enumerate(
            ((w_drive, v_drive), (w_open, v_open), (w_glu, v_glu), (w_merge, v_merge), (w_exit, v_exit))
        ):
            loads[i, l] = load(src.at[l], dst.at[l], w_sem.at[i, l])

    def weight(i, l):
        if (i, l) in loads:
            loads.pop((i, l)).wait()

    pending = []

    def send(src, dst, ss, rs, to_dp, to_tp, is_self):
        far = pltpu.make_async_remote_copy(
            src_ref=src, dst_ref=dst, send_sem=ss, recv_sem=rs,
            device_id={"tp": to_tp, "dp": to_dp}, device_id_type=pl.DeviceIdType.MESH,
        )
        if is_self is None:
            far.start()
        else:
            @pl.when(is_self)
            def _():
                pltpu.make_async_copy(src, dst, rs).start()

            @pl.when(jnp.logical_not(is_self))
            def _():
                far.start()

        pending.append((far, is_self))

    def arrive(dst, rs):
        pltpu.make_async_copy(dst, dst, rs).wait()

    def send_row(k, c):
        send(row_send.at[k, c], row_recv.at[k, d], row_ss.at[k, c], row_rs.at[k, d], c, t, d == c)

    def row_sum(k):
        acc = None
        for s in range(nd):
            arrive(row_recv.at[k, s], row_rs.at[k, s])
            v = row_recv[k, s].astype(f32)
            acc = v if acc is None else acc + v
        return acc

    def send_rows(k, part):
        part = part.astype(bf16)
        for c in range(nd):
            row_send[k, c] = part[c * chunk:(c + 1) * chunk]
            send_row(k, c)

    def spread_x(k):
        slot = place * nd + d
        for j in range(nd):
            to = lax.rem(home + j, nd) * ratio + place
            send(
                x_src.at[k], x_recv.at[k, place, pl.ds(d * chunk, chunk)],
                x_ss.at[k, j], x_rs.at[k, slot], home, to, (d == home) if j == 0 else None,
            )

    def forward_x(k):
        for s in range(nd):
            piece = x_recv.at[k, place, pl.ds(s * chunk, chunk)]
            arrive(piece, x_rs.at[k, place * nd + s])
            for i in range(1, ratio):
                to = home * ratio + lax.rem(place + i, ratio)
                send(
                    piece, piece, x_ss.at[k, nd + s * (ratio - 1) + i - 1],
                    x_rs.at[k, place * nd + s], d, to, None,
                )

    def take_x(k):
        for i in range(1, ratio):
            p = lax.rem(place + i, ratio)
            for s in range(nd):
                arrive(x_recv.at[k, p, pl.ds(s * chunk, chunk)], x_rs.at[k, p * nd + s])

    def spread_y(k):
        slot = place * nd + d
        for j in range(nd):
            to = lax.rem(home + j, nd) * ratio + place
            send(
                y_src.at[k], y_recv.at[k, slot],
                y_ss.at[k, j], y_rs.at[k, slot], home, to, (d == home) if j == 0 else None,
            )

    def forward_y(k):
        for s in range(nd):
            slot = place * nd + s
            piece = y_recv.at[k, slot]
            arrive(piece, y_rs.at[k, slot])
            for i in range(1, ratio):
                to = home * ratio + lax.rem(place + i, ratio)
                send(
                    piece, piece, y_ss.at[k, nd + s * (ratio - 1) + i - 1],
                    y_rs.at[k, slot], d, to, None,
                )

    def take_y(k):
        for i in range(1, ratio):
            p = lax.rem(place + i, ratio)
            for s in range(nd):
                arrive(y_recv.at[k, p * nd + s], y_rs.at[k, p * nd + s])
        parts = []
        for p in range(ratio):
            for s in range(nd):
                v = y_recv[k, p * nd + s]
                parts.append(jnp.concatenate([v[:, :width], v[:, width:]], axis=0))
        return jnp.concatenate(parts, axis=1)

    def fold(v):
        return jnp.concatenate([v[:half], v[half:]], axis=1)

    def send_states(l):
        for c in range(nd):
            send(
                carried.at[l, :, :, pl.ds(c * own_ch, own_ch)], st_recv.at[l, d],
                st_ss.at[l, c], st_rs.at[l, d], c, t, d == c,
            )

    def return_states(l):
        for c in range(nd):
            send(
                st_new.at[l, :, pl.ds(c * batch_own, batch_own)],
                out_state.at[l, :, :, pl.ds(pl.multiple_of(d * own_ch, own_ch), own_ch)],
                n_ss.at[l, c], n_rs.at[l, d], c, t, d == c,
            )

    wide = jnp.concatenate([lens[...].astype(f32)] * nd, axis=1)
    owner = lax.broadcasted_iota(jnp.int32, wide.shape, 1) // batch_own
    len_own[...] = jnp.broadcast_to(jnp.where(owner == d, wide, 0.0), len_own.shape)

    def upright_of(v, n):
        a = lax.broadcasted_iota(jnp.int32, (n, n), 0)
        b = lax.broadcasted_iota(jnp.int32, (n, n), 1)
        return jnp.sum(jnp.where(a == b, jnp.broadcast_to(v, (n, n)), 0.0), axis=1, keepdims=True)

    for l in range(layers):
        real_eig, turn_now = -rate[l], turn[l]
        step_len = upright_of(size[l:l + 1, :], size.shape[1])
        magnitude = jnp.exp(step_len * real_eig)
        decay_real = magnitude * jnp.cos(step_len * turn_now)
        decay_imag = magnitude * jnp.sin(step_len * turn_now)
        divisor = real_eig * real_eig + turn_now * turn_now
        par[l, 0] = decay_real
        par[l, 1] = decay_imag
        par[l, 2] = ((decay_real - 1.0) * real_eig + decay_imag * turn_now) / divisor
        par[l, 3] = (decay_imag * real_eig - (decay_real - 1.0) * turn_now) / divisor

    pl.semaphore_wait(barrier, total - 1)
    for c in range(nd):
        send(len_own, len_recv.at[d], l_ss.at[c], l_rs.at[d], c, t, d == c)

    in_load.wait()
    out_load.wait()

    def blocks(j, a, b):
        blank = jnp.zeros((members, entries), f32)
        row = [blank] * j + [a] + [blank] * (few - 1 - j) + [blank] * j + [b] + [blank] * (few - 1 - j)
        return jnp.concatenate(row, axis=1).astype(bf16)

    for l in range(layers):
        for j in range(few):
            hold_real = par[l, 2, pl.ds(d * few + j, 1), :]
            hold_imag = par[l, 3, pl.ds(d * few + j, 1), :]
            a, b = v_in[l, 0, j], v_in[l, 1, j]
            inj[l, j * members:(j + 1) * members, :] = blocks(
                j, hold_real * a - hold_imag * b, hold_real * b + hold_imag * a
            )
            omx[l, j * members:(j + 1) * members, :] = blocks(j, v_out[l, 0, j], -v_out[l, 1, j])
        inj[l, width:, :] = jnp.zeros((width, 2 * own_ch), bf16)
        omx[l, width:, :] = jnp.zeros((width, 2 * own_ch), bf16)

    def decays(l, part):
        return jnp.concatenate([par[l, part, pl.ds(d * few + j, 1), :] for j in range(few)], axis=1)

    def skips(l):
        own = None
        for s in range(nd):
            v = skip[l:l + 1, s * width:(s + 1) * width]
            own = v if own is None else jnp.where(d == s, v, own)
        return jnp.concatenate([own, jnp.zeros_like(own)], axis=1)

    len_row = None
    for s in range(nd):
        arrive(len_recv.at[s], l_rs.at[s])
        len_row = len_recv[s] if len_row is None else len_row + len_recv[s]
    down = lax.broadcasted_iota(jnp.int32, (batch, batch), 0)
    along = lax.broadcasted_iota(jnp.int32, (batch, batch), 1)
    before = jnp.where(down < along, 1.0, 0.0).astype(bf16)
    start_row = jnp.dot(len_row.astype(bf16), before, preferred_element_type=f32)

    local = lax.broadcasted_iota(jnp.int32, (batch, own_rows), 0) - d * batch_own
    item = lax.broadcasted_iota(jnp.int32, (batch, own_rows), 1)
    inside = jnp.logical_and(item >= local * steps, item < (local + 1) * steps)
    expand = jnp.where(inside, 1.0, 0.0)
    order = (lax.broadcasted_iota(jnp.int32, len_row.shape, 1) - d * batch_own).astype(f32)
    exact = functools.partial(
        jnp.dot, preferred_element_type=f32, precision=lax.Precision.HIGHEST
    )
    spot = exact(start_row - steps * order, expand)[0:1]
    spot = spot + lax.broadcasted_iota(jnp.int32, (1, own_rows), 1).astype(f32)
    end = exact(start_row + len_row, expand)[0:1]
    spot = jnp.where(spot < end, spot, -1.0)
    tall = lax.broadcasted_iota(jnp.int32, (all_rows, own_rows), 0).astype(f32)
    pack_own[...] = jnp.where(tall == spot, 1.0, 0.0).astype(bf16)

    def turned(a, b):
        return lax.dot_general(a, b, (((0,), (0,)), ((), ())), preferred_element_type=f32)

    every = range(lots)
    tok_load.wait()
    for h in every:
        send_rows(h, jnp.dot(
            pack_own[h * rows:(h + 1) * rows, :], v_tok[...], preferred_element_type=f32
        ))

    len_col, start_col = upright_of(len_row[0:1], batch), upright_of(start_row[0:1], batch)
    count = lax.broadcasted_iota(jnp.int32, (batch, all_rows), 1).astype(f32)
    for step in range(steps):
        hit = jnp.logical_and(count == start_col + step, len_col > step)
        unpack[step * batch:(step + 1) * batch, :] = jnp.where(hit, 1.0, 0.0).astype(bf16)

    def begin(h):
        x_src[h] = row_sum(h).astype(bf16)
        spread_x(h)
        yield
        yield from enter(0, h)

    def enter(l, h):
        k = 2 * l * lots + h
        forward_x(k)
        yield
        weight(0, l)
        take_x(k)
        squares = None
        for p in range(ratio):
            raw = x_recv[k, p].astype(f32)
            sq = jnp.sum(raw * raw, axis=1, keepdims=True)
            squares = sq if squares is None else squares + sq
            gain = gains[l:l + 1, pl.ds(pl.multiple_of((d * ratio + p) * cols, cols), cols)]
            norm_buf[h, :, p * cols:(p + 1) * cols] = (raw * gain).astype(bf16)
        drive = jnp.dot(norm_buf[h], v_drive[l], preferred_element_type=f32)
        high = squares.astype(bf16)
        low = (squares - high.astype(f32)).astype(bf16)
        lane = lax.broadcasted_iota(jnp.int32, (rows, width), 1)
        tail = jnp.where(
            lane == 0, high.astype(f32), jnp.where(lane == 1, low.astype(f32), 0.0)
        ).astype(bf16)
        k = l * lots + h
        for c in range(nd):
            a_send[k, c] = jnp.concatenate(
                [drive[:, c * width:(c + 1) * width].astype(bf16), tail], axis=1
            )
            send(a_send.at[k, c], a_recv.at[k, d], a_ss.at[k, c], a_rs.at[k, d], c, t, d == c)
        yield
        weight(1, l)
        send_rows(
            (1 + 3 * l) * lots + h, jnp.dot(norm_buf[h], v_open[l], preferred_element_type=f32)
        )
        yield

    def recur(l):
        for h in every:
            k = l * lots + h
            summed = None
            for s in range(nd):
                arrive(a_recv.at[k, s], a_rs.at[k, s])
                v = a_recv[k, s].astype(f32)
                summed = v if summed is None else summed + v
            full_sq = summed[:, width:width + 1] + summed[:, width + 1:width + 2]
            inverse = lax.rsqrt(full_sq / model + EPS)
            inv_buf[h * rows:(h + 1) * rows, :] = jnp.broadcast_to(inverse, (rows, 128))
            lane = lax.broadcasted_iota(jnp.int32, summed.shape, 1)
            feed = jnp.where(lane < width, summed * inverse, jnp.where(lane == width, 1.0, 0.0))
            feed_buf[h * rows:(h + 1) * rows, :] = feed.astype(bf16)
        for s in range(nd):
            arrive(st_recv.at[l, s], st_rs.at[l, s])
        real = jnp.concatenate([st_recv[l, s, 0] for s in range(nd)], axis=0)
        imag = jnp.concatenate([st_recv[l, s, 1] for s in range(nd)], axis=0)
        dr, di, gap = decays(l, 0), decays(l, 1), skips(l)
        for step in range(steps):
            span = slice(step * batch, (step + 1) * batch)
            u = jnp.dot(unpack[span, :], feed_buf[...], preferred_element_type=f32)
            live = u[:, width:width + 1] > 0.5
            push = jnp.dot(u.astype(bf16), inj[l], preferred_element_type=f32)
            moved_real = dr * real - di * imag + push[:, :own_ch]
            moved_imag = dr * imag + di * real + push[:, own_ch:]
            real = jnp.where(live, moved_real, real)
            imag = jnp.where(live, moved_imag, imag)
            both = jnp.concatenate([real, imag], axis=1).astype(bf16)
            read = lax.dot_general(
                both, omx[l], (((1,), (1,)), ((), ())), preferred_element_type=f32
            ) + gap * u
            act_buf[span, :] = jax.nn.gelu(read).astype(bf16)
        st_new[l, 0] = real
        st_new[l, 1] = imag

    def chain(l, h):
        first, second = 2 * l * lots + h, (2 * l + 1) * lots + h
        k_open = (1 + 3 * l) * lots + h
        k_merge, k_exit = k_open + lots, k_open + 2 * lots
        packed = turned(unpack[:, h * rows:(h + 1) * rows], act_buf[...]).astype(bf16)
        y_src[first] = fold(packed[:, :width])
        spread_y(first)
        yield
        forward_y(first)
        yield
        weight(2, l)
        gating = jnp.dot(take_y(first), v_glu[l], preferred_element_type=f32).astype(bf16)
        k = l * lots + h
        for c in range(nd):
            c_send[k, c] = fold(gating[:, c * width:(c + 1) * width])
            send(c_send.at[k, c], c_recv.at[k, d], c_ss.at[k, c], c_rs.at[k, d], c, t, d == c)
        yield
        summed = None
        for s in range(nd):
            arrive(c_recv.at[k, s], c_rs.at[k, s])
            v = c_recv[k, s].astype(f32)
            summed = v if summed is None else summed + v
        y_src[second] = (y_src[first].astype(f32) * jax.nn.sigmoid(summed)).astype(bf16)
        spread_y(second)
        yield
        forward_y(second)
        yield
        weight(3, l)
        send_rows(k_merge, jnp.dot(take_y(second), v_merge[l], preferred_element_type=f32))
        yield
        mine = pl.ds(pl.multiple_of(h * rows + d * chunk, chunk), chunk)
        gate = jax.nn.sigmoid(row_sum(k_open) * inv_buf[mine, 0:1])
        x_src[second] = (gate * row_sum(k_merge)).astype(bf16)
        spread_x(second)
        yield
        forward_x(second)
        yield
        weight(4, l)
        take_x(second)
        part = None
        for p in range(ratio):
            v = jnp.dot(
                x_recv[second, p], v_exit[l, p * cols:(p + 1) * cols], preferred_element_type=f32
            )
            part = v if part is None else part + v
        send_rows(k_exit, part)
        yield
        k = (2 * l + 2) * lots + h
        x_src[k] = (x_src[first].astype(f32) + row_sum(k_exit)).astype(bf16)
        if l + 1 < layers:
            spread_x(k)
            yield
            yield from enter(l + 1, h)
        else:
            for c in range(nd):
                send(
                    x_src.at[k], fin_recv.at[pl.ds(h * rows + d * chunk, chunk)],
                    f_ss.at[h, c], f_rs.at[h, d], c, t, d == c,
                )
            yield

    def run(gens, hooks):
        live, turn_count = list(range(lots)), 0
        while live:
            for h in list(live):
                if turn_count >= h * SKEW:
                    try:
                        next(gens[h])
                    except StopIteration:
                        live.remove(h)
            if turn_count in hooks:
                hooks.pop(turn_count)()
            turn_count += 1
        for rest in hooks.values():
            rest()

    run([begin(h) for h in every], {2 * SKEW: lambda: send_states(0)})
    for l in range(layers):
        recur(l)
        hooks = {4: functools.partial(return_states, l)}
        if l + 1 < layers:
            hooks[7] = functools.partial(send_states, l + 1)
        run([chain(l, h) for h in every], hooks)
    for l in range(layers):
        for s in range(nd):
            into = out_state.at[l, :, :, pl.ds(s * own_ch, own_ch)]
            arrive(into, n_rs.at[l, s])
    for h in every:
        for s in range(nd):
            arrive(fin_recv.at[pl.ds(h * rows + s * chunk, chunk)], f_rs.at[h, s])
    spread = turned(pack_own[...], fin_recv[...])
    keep = turned(pack_own[...], jnp.ones((all_rows, 128), bf16))[:, 0:1]
    out_tok[...] = jnp.where(keep > 0.5, spread, v_tok[...].astype(f32)).astype(bf16)
    for far, is_self in pending:
        if is_self is None:
            far.wait_send()
        else:
            pl.when(jnp.logical_not(is_self))(far.wait_send)


def fused_shards(
    tokens, lengths, norm_gains, drive_proj, open_proj, glu_proj, merge_proj, exit_proj,
    decay_rate, turn_rate, group_step_width, state_in, state_out, skip_gain, carried_state,
):
    f32, bf16 = jnp.float32, jnp.bfloat16
    nd, nt = lax.axis_size("dp"), lax.axis_size("tp")
    layers = norm_gains.shape[0]
    own, steps, cols = tokens.shape
    batch = own * nd
    rows = 3 * batch
    model = cols * nt
    ratio = nt // nd
    groups_own = decay_rate.shape[1]
    few = groups_own // nd
    entries = decay_rate.shape[2]
    members = state_in.shape[-1]
    width = few * members
    own_ch = few * entries
    chunk = rows // nd

    lots = LOTS
    n_row = (1 + 3 * layers) * lots
    n_col = layers * lots
    n_all = 2 * layers * lots
    lot = rows // lots
    piece = chunk // lots
    half = lot // 2
    vm = pltpu.VMEM
    dma = pltpu.SemaphoreType.DMA
    weights = (drive_proj, open_proj, glu_proj, merge_proj, exit_proj)
    scratch = [vm(w.shape, bf16) for w in weights] + [
        vm((own * steps, cols), bf16),
        vm((layers, 2, few, members, entries), f32),
        vm((layers, 2, few, members, entries), f32),
        vm((layers, 4, groups_own, entries), f32),
        vm((layers, 2 * width, 2 * own_ch), bf16),
        vm((layers, 2 * width, 2 * own_ch), bf16),
        vm((8, batch), f32),
        vm((n_row, nd, piece, cols), bf16),
        vm((n_row, nd, piece, cols), bf16),
        vm((n_col, nd, lot, 2 * width), bf16),
        vm((n_col, nd, lot, 2 * width), bf16),
        vm((n_col, nd, half, 2 * width), bf16),
        vm((n_col, nd, half, 2 * width), bf16),
        vm((n_all + lots, piece, cols), bf16),
        vm((n_all, ratio, lot, cols), bf16),
        vm((n_all, half, 2 * width), bf16),
        vm((n_all, nt, half, 2 * width), bf16),
        vm((layers, nd, 2, own, own_ch), f32),
        vm((layers, 2, batch, own_ch), f32),
        vm((rows, cols), bf16),
        vm((lots, lot, ratio * cols), bf16),
        vm((rows, 128), f32),
        vm((steps * batch, 2 * width), bf16),
        vm((rows, 2 * width), bf16),
        vm((nd, 8, batch), f32),
        vm((rows, own * steps), bf16),
        vm((steps * batch, rows), bf16),
        dma((5, layers)), dma((3,)),
        dma((n_row, nd)), dma((n_row, nd)),
        dma((n_col, nd)), dma((n_col, nd)),
        dma((n_col, nd)), dma((n_col, nd)),
        dma((n_all, nd * ratio)), dma((n_all, nt)),
        dma((n_all, nd * ratio)), dma((n_all, nt)),
        dma((layers, nd)), dma((layers, nd)),
        dma((layers, nd)), dma((layers, nd)),
        dma((lots, nd)), dma((lots, nd)),
        dma((nd,)), dma((nd,)),
    ]
    inside = pl.BlockSpec(memory_space=pltpu.VMEM)
    outside = pl.BlockSpec(memory_space=pl.ANY)
    out_rows, out_state = pl.pallas_call(
        functools.partial(fused_kernel, (layers, nd, nt, rows, model, lots)),
        out_shape=(
            jax.ShapeDtypeStruct((own * steps, cols), bf16),
            jax.ShapeDtypeStruct(carried_state.shape, f32),
        ),
        in_specs=[outside] + [inside] * 5 + [outside] * 2 + [inside] + [outside] * 6,
        out_specs=(inside, outside),
        scratch_shapes=scratch,
        compiler_params=pltpu.CompilerParams(
            collective_id=0, has_side_effects=True, vmem_limit_bytes=60 * 1024 * 1024
        ),
    )(
        tokens.reshape(own * steps, cols), lengths.reshape(1, own),
        norm_gains, decay_rate, turn_rate, group_step_width,
        jnp.swapaxes(state_in, 3, 4), state_out, skip_gain, carried_state, *weights,
    )
    return out_rows.reshape(own, steps, cols), out_state


def solution(mesh):
    in_specs = (
        P("dp", None, "tp"),
        P("dp"),
        P(),
        P(None, "dp", "tp"),
        P(None, "dp", "tp"),
        P(None, "dp", "tp"),
        P(None, "dp", "tp"),
        P(None, "dp", "tp"),
        P(None, "tp", None),
        P(None, "tp", None),
        P(None, "tp"),
        P(None, None, "tp", None, None),
        P(None, None, "tp", None, None),
        P(None, "tp"),
        P(None, None, "dp", "tp"),
    )
    out_specs = (P("dp", None, "tp"), P(None, None, "dp", "tp"))
    ways, nd = mesh.shape["tp"], mesh.shape["dp"]

    def run(*args):
        groups = args[8].shape[1] // ways
        whole_groups = groups % nd == 0 and ways % nd == 0
        body = fused_shards if whole_groups else shards
        return jax.shard_map(body, mesh=mesh, in_specs=in_specs, out_specs=out_specs, check_vma=False)(*args)

    return run
```

```python
import functools
import jax
import jax.numpy as jnp
from jax import lax
from jax.experimental import pallas as pl
from jax.experimental.pallas import tpu as pltpu
from jax.sharding import PartitionSpec as P

EPS = 1e-05


def state_update(
    drive, active, current_rate, turn_now, size_now, in_pair, output_couple, skip_now, carried
):
    sequences, positions = active.shape
    groups, entries = current_rate.shape
    members = in_pair.shape[-1]
    real_eig = -current_rate
    step_len = size_now[:, None]
    magnitude = jnp.exp(step_len * real_eig)
    decay_real = magnitude * jnp.cos(step_len * turn_now)
    decay_imag = magnitude * jnp.sin(step_len * turn_now)
    divisor = real_eig * real_eig + turn_now * turn_now
    hold_real = ((decay_real - 1.0) * real_eig + decay_imag * turn_now) / divisor
    hold_imag = (decay_imag * real_eig - (decay_real - 1.0) * turn_now) / divisor
    inject_real = hold_real[..., None] * in_pair[0] - hold_imag[..., None] * in_pair[1]
    inject_imag = hold_real[..., None] * in_pair[1] + hold_imag[..., None] * in_pair[0]
    inputs = drive.reshape(sequences, positions, groups, members)
    pushed_real = jnp.einsum("gpc,bsgc->bsgp", inject_real, inputs, precision=lax.Precision.HIGHEST)
    pushed_imag = jnp.einsum("gpc,bsgc->bsgp", inject_imag, inputs, precision=lax.Precision.HIGHEST)
    state_real_part = carried[0].reshape(sequences, groups, entries)
    state_imaginary = carried[1].reshape(sequences, groups, entries)
    readings = []
    for position in range(positions):
        active_now = (active[:, position] > 0)[:, None, None]
        moved_real = (
            decay_real * state_real_part - decay_imag * state_imaginary + pushed_real[:, position]
        )
        moved_imag = (
            decay_real * state_imaginary + decay_imag * state_real_part + pushed_imag[:, position]
        )
        state_real_part = jnp.where(active_now, moved_real, state_real_part)
        state_imaginary = jnp.where(active_now, moved_imag, state_imaginary)
        readout_value = jnp.einsum(
            "sal,usl->usa", output_couple[0], state_real_part, precision=lax.Precision.HIGHEST
        ) - jnp.einsum(
            "sal,usl->usa", output_couple[1], state_imaginary, precision=lax.Precision.HIGHEST
        )
        readings.append(readout_value)
    readout = jnp.stack(readings, axis=1) + skip_now.reshape(groups, members) * inputs
    final = jnp.stack(
        [
            state_real_part.reshape(sequences, groups * entries),
            state_imaginary.reshape(sequences, groups * entries),
        ]
    )
    return (readout.reshape(sequences * positions, groups * members), final)


def widen_model(values):
    return lax.all_gather(values, "tp", axis=1, tiled=True)


def widen_branch(values):
    return lax.all_gather(values, "tp", axis=1, tiled=True)


def project(gathered, weight):
    return jnp.dot(
        gathered,
        lax.all_gather(weight, "dp", axis=0, tiled=True),
        preferred_element_type=jnp.float32,
    )


def shards(
    tokens,
    lengths,
    norm_gains,
    drive_proj,
    open_proj,
    glu_proj,
    merge_proj,
    exit_proj,
    decay_rate,
    turn_rate,
    group_step_width,
    state_in,
    state_out,
    skip_gain,
    carried_state,
):
    sequences, positions, local_width = tokens.shape
    row_count = sequences * positions
    model_width = local_width * lax.axis_size("tp")
    first_col = lax.axis_index("tp") * local_width
    active = (lax.broadcasted_iota(jnp.int32, (sequences, positions), 1) < lengths[:, None]).astype(
        jnp.int32
    )
    active_rows = active.reshape(row_count, 1).astype(jnp.float32)
    residual = tokens.reshape(row_count, local_width)
    states = []
    for layer_index in range(norm_gains.shape[0]):
        norm_gain = norm_gains[layer_index]
        own_values = residual.astype(jnp.float32)
        squared_sum = lax.psum(jnp.sum(own_values * own_values, axis=1), "tp")
        inverse_rms = lax.rsqrt(squared_sum / model_width + EPS)[:, None]
        own_gain = lax.dynamic_slice_in_dim(norm_gain, first_col, local_width, 0)
        gathered = widen_model((own_values * inverse_rms * own_gain).astype(jnp.bfloat16))
        drive = project(gathered, drive_proj[layer_index])
        gate_open = jax.nn.sigmoid(project(gathered, open_proj[layer_index]))
        readout, final = state_update(
            drive,
            active,
            decay_rate[layer_index],
            turn_rate[layer_index],
            group_step_width[layer_index],
            state_in[layer_index],
            state_out[layer_index],
            skip_gain[layer_index],
            carried_state[layer_index],
        )
        states.append(final)
        activated = jax.nn.gelu(readout).astype(jnp.bfloat16)
        gating = project(widen_branch(activated), glu_proj[layer_index])
        gated = (activated.astype(jnp.float32) * jax.nn.sigmoid(gating)).astype(jnp.bfloat16)
        merged = project(widen_branch(gated), merge_proj[layer_index])
        mixed = (gate_open * merged).astype(jnp.bfloat16)
        branch = project(widen_model(mixed), exit_proj[layer_index])
        residual = (residual.astype(jnp.float32) + active_rows * branch).astype(jnp.bfloat16)
    return (residual.reshape(sequences, positions, local_width), jnp.stack(states))


LOTS = 6
MIXED = 1
ROW, COL, ST, LEN, FIN, XF, YF, LANES = 0, 1, 3, 5, 6, 7, 13, 19


def fused_kernel(
    dims,
    tok, lens, gains, rate, turn, size, s_in, s_out, skip, carried,
    w_drive, w_open, w_glu, w_merge, w_exit,
    out_tok, out_state,
    v_drive, v_open, v_glu, v_merge, v_exit, v_tok, v_in, v_out,
    par, inj, omx, len_own,
    row_send, row_recv, a_send, a_recv, c_send, c_recv,
    x_src, x_near, x_recv, y_src, y_near, y_recv, st_recv, st_new, fin_recv,
    norm_buf, inv_buf, act_buf, feed_buf, len_recv, pack_own, unpack,
    w_sem, in_sem, row_rs, a_rs, c_rs, x_rs, y_rs, xn_rs, yn_rs, st_rs, n_rs, f_rs, l_rs, out_sem,
):
    layers, nd, nt, all_rows, model, lots = dims
    ratio = nt // nd
    rows = all_rows // lots
    chunk = rows // nd
    half = rows // 2
    f32, bf16 = jnp.float32, jnp.bfloat16
    d = lax.axis_index("dp")
    t = lax.axis_index("tp")
    home = t // ratio
    place = lax.rem(t, ratio)
    batch_own = carried.shape[2]
    batch = batch_own * nd
    few, members, entries = v_in.shape[2:]
    own_ch = few * entries
    width = few * members
    own_rows = v_tok.shape[0]
    steps = own_rows // batch_own
    cols = v_tok.shape[1]

    def load(src, dst, sem):
        copy = pltpu.make_async_copy(src, dst, sem)
        copy.start()
        return copy

    tok_load = load(tok, v_tok, in_sem.at[0])
    in_load = load(s_in.at[:, :, pl.ds(d * few, few)], v_in, in_sem.at[1])
    out_load = load(s_out.at[:, :, pl.ds(d * few, few)], v_out, in_sem.at[2])

    barrier = pltpu.get_barrier_semaphore()
    total = nd * nt
    flat = t * nd + d

    def greet(i, carry):
        other = lax.rem(flat + i, total)
        pl.semaphore_signal(
            barrier, inc=1,
            device_id={"tp": other // nd, "dp": lax.rem(other, nd)},
            device_id_type=pl.DeviceIdType.MESH,
        )
        return carry

    lax.fori_loop(1, total, greet, 0)

    loads = {}
    for l in range(layers):
        for i, (src, dst) in enumerate(
            ((w_drive, v_drive), (w_open, v_open), (w_glu, v_glu), (w_merge, v_merge), (w_exit, v_exit))
        ):
            loads[i, l] = load(src.at[l], dst.at[l], w_sem.at[i, l])

    def weight(i, l):
        if (i, l) in loads:
            loads.pop((i, l)).wait()

    def send(src, dst, rs, to_dp, to_tp, lane):
        copy = pltpu.make_async_remote_copy(
            src_ref=src, dst_ref=dst, send_sem=out_sem.at[lane], recv_sem=rs,
            device_id={"tp": to_tp, "dp": to_dp}, device_id_type=pl.DeviceIdType.MESH,
        )
        copy.start()

    def arrive(dst, rs):
        pltpu.make_async_copy(dst, dst, rs).wait()

    others = [(j, lax.rem(d + j, nd)) for j in range(1, nd)]

    def trade(src, dst, rs, lane):
        for j, to in others:
            send(src.at[to], dst.at[j - 1], rs, to, t, lane)

    def traded(src, dst, rs):
        arrive(dst, rs)
        acc = src[d].astype(f32)
        for j in range(nd - 1):
            acc = acc + dst[j].astype(f32)
        return acc

    def row_sum(k):
        return traded(row_send.at[k], row_recv.at[k], row_rs.at[k])

    def send_rows(k, part):
        part = part.astype(bf16)
        for c in range(nd):
            row_send[k, c] = part[c * chunk:(c + 1) * chunk]
        trade(row_send.at[k], row_recv.at[k], row_rs.at[k], ROW)

    def fan(src, dst, rs, lane):
        for j in range(1, nd):
            send(src, dst, rs, home, lax.rem(home + j, nd) * ratio + place, lane)

        @pl.when(d == home)
        def _():
            pltpu.make_async_copy(src, dst, rs).start()

        @pl.when(d != home)
        def _():
            send(src, dst, rs, home, t, lane + 1)

    def aside(src, near, rs, lane):
        for i in range(1, ratio):
            p = lax.rem(place + i, ratio)
            send(src, near.at[i - 1], rs.at[i - 1], d, home * ratio + p, lane)

    def x_slot(k, p):
        return x_recv.at[k, p, pl.ds(d * chunk, chunk)]

    def y_slot(k, p):
        return y_recv.at[k, p * nd + d]

    def x_whole(k, p):
        return x_recv.at[k, p]

    def y_whole(k, p):
        return y_recv.at[k, pl.ds(p * nd, nd)]

    X = (x_src, x_near, x_slot, x_whole, x_rs, xn_rs, XF)
    Y = (y_src, y_near, y_slot, y_whole, y_rs, yn_rs, YF)

    def spread(kind, k, near_first):
        src, near, slot, whole, rs, near_rs, lane = kind
        if near_first:
            aside(src.at[k], near.at[k], near_rs.at[k], lane + 3)
        else:
            fan(src.at[k], slot(k, place), rs.at[k, place], lane)

    def forward(kind, k, near_first):
        src, near, slot, whole, rs, near_rs, lane = kind
        if near_first:
            fan(src.at[k], slot(k, place), rs.at[k, place], lane)
            for i in range(1, ratio):
                p = lax.rem(place + ratio - i, ratio)
                arrive(near.at[k, i - 1], near_rs.at[k, i - 1])
                fan(near.at[k, i - 1], slot(k, p), rs.at[k, p], lane + 4)
        else:
            arrive(whole(k, place), rs.at[k, place])
            for i in range(1, ratio):
                to = home * ratio + lax.rem(place + i, ratio)
                send(whole(k, place), whole(k, place), rs.at[k, place], d, to, lane + 2)

    def take(kind, k, near_first):
        src, near, slot, whole, rs, near_rs, lane = kind
        for i in range(0 if near_first else 1, ratio):
            p = lax.rem(place + i, ratio)
            arrive(whole(k, p), rs.at[k, p])

    def take_y(k, near_first):
        take(Y, k, near_first)
        parts = []
        for p in range(ratio):
            for s in range(nd):
                v = y_recv[k, p * nd + s]
                parts.append(jnp.concatenate([v[:, :width], v[:, width:]], axis=0))
        return jnp.concatenate(parts, axis=1)

    def fold(v):
        return jnp.concatenate([v[:half], v[half:]], axis=1)

    def own_span(c):
        return pl.ds(pl.multiple_of(c * own_ch, own_ch), own_ch)

    def send_states(l):
        into = st_recv.at[l, d]
        pltpu.make_async_copy(carried.at[l, :, :, own_span(d)], into, st_rs.at[l]).start()
        for j, to in others:
            send(carried.at[l, :, :, own_span(to)], into, st_rs.at[l], to, t, ST)

    def return_states(l):
        def rows_of(c):
            return st_new.at[l, :, pl.ds(pl.multiple_of(c * batch_own, batch_own), batch_own)]

        into = out_state.at[l, :, :, own_span(d)]
        pltpu.make_async_copy(rows_of(d), into, n_rs.at[l]).start()
        for j, to in others:
            send(rows_of(to), into, n_rs.at[l], to, t, ST + 1)

    wide = jnp.concatenate([lens[...].astype(f32)] * nd, axis=1)
    owner = lax.broadcasted_iota(jnp.int32, wide.shape, 1) // batch_own
    len_own[...] = jnp.broadcast_to(jnp.where(owner == d, wide, 0.0), len_own.shape)

    def upright_of(v, n):
        a = lax.broadcasted_iota(jnp.int32, (n, n), 0)
        b = lax.broadcasted_iota(jnp.int32, (n, n), 1)
        return jnp.sum(jnp.where(a == b, jnp.broadcast_to(v, (n, n)), 0.0), axis=1, keepdims=True)

    for l in range(layers):
        real_eig, turn_now = -rate[l], turn[l]
        step_len = upright_of(size[l:l + 1, :], size.shape[1])
        magnitude = jnp.exp(step_len * real_eig)
        decay_real = magnitude * jnp.cos(step_len * turn_now)
        decay_imag = magnitude * jnp.sin(step_len * turn_now)
        divisor = real_eig * real_eig + turn_now * turn_now
        par[l, 0] = decay_real
        par[l, 1] = decay_imag
        par[l, 2] = ((decay_real - 1.0) * real_eig + decay_imag * turn_now) / divisor
        par[l, 3] = (decay_imag * real_eig - (decay_real - 1.0) * turn_now) / divisor

    pl.semaphore_wait(barrier, total - 1)
    for j, to in others:
        send(len_own, len_recv.at[j - 1], l_rs.at[0], to, t, LEN)

    in_load.wait()
    out_load.wait()

    def blocks(j, a, b):
        blank = jnp.zeros((members, entries), f32)
        row = [blank] * j + [a] + [blank] * (few - 1 - j) + [blank] * j + [b] + [blank] * (few - 1 - j)
        return jnp.concatenate(row, axis=1).astype(bf16)

    for l in range(layers):
        for j in range(few):
            hold_real = par[l, 2, pl.ds(d * few + j, 1), :]
            hold_imag = par[l, 3, pl.ds(d * few + j, 1), :]
            a, b = v_in[l, 0, j], v_in[l, 1, j]
            inj[l, j * members:(j + 1) * members, :] = blocks(
                j, hold_real * a - hold_imag * b, hold_real * b + hold_imag * a
            )
            omx[l, j * members:(j + 1) * members, :] = blocks(j, v_out[l, 0, j], -v_out[l, 1, j])
        inj[l, width:, :] = jnp.zeros((width, 2 * own_ch), bf16)
        omx[l, width:, :] = jnp.zeros((width, 2 * own_ch), bf16)

    def decays(l, part):
        return jnp.concatenate([par[l, part, pl.ds(d * few + j, 1), :] for j in range(few)], axis=1)

    def skips(l):
        own = None
        for s in range(nd):
            v = skip[l:l + 1, s * width:(s + 1) * width]
            own = v if own is None else jnp.where(d == s, v, own)
        return jnp.concatenate([own, jnp.zeros_like(own)], axis=1)

    arrive(len_recv, l_rs.at[0])
    len_row = len_own[...]
    for s in range(nd - 1):
        len_row = len_row + len_recv[s]
    down = lax.broadcasted_iota(jnp.int32, (batch, batch), 0)
    along = lax.broadcasted_iota(jnp.int32, (batch, batch), 1)
    before = jnp.where(down < along, 1.0, 0.0).astype(bf16)
    start_row = jnp.dot(len_row.astype(bf16), before, preferred_element_type=f32)

    local = lax.broadcasted_iota(jnp.int32, (batch, own_rows), 0) - d * batch_own
    item = lax.broadcasted_iota(jnp.int32, (batch, own_rows), 1)
    inside = jnp.logical_and(item >= local * steps, item < (local + 1) * steps)
    expand = jnp.where(inside, 1.0, 0.0)
    order = (lax.broadcasted_iota(jnp.int32, len_row.shape, 1) - d * batch_own).astype(f32)
    exact = functools.partial(
        jnp.dot, preferred_element_type=f32, precision=lax.Precision.HIGHEST
    )
    spot = exact(start_row - steps * order, expand)[0:1]
    spot = spot + lax.broadcasted_iota(jnp.int32, (1, own_rows), 1).astype(f32)
    end = exact(start_row + len_row, expand)[0:1]
    spot = jnp.where(spot < end, spot, -1.0)
    tall = lax.broadcasted_iota(jnp.int32, (all_rows, own_rows), 0).astype(f32)
    pack_own[...] = jnp.where(tall == spot, 1.0, 0.0).astype(bf16)

    def turned(a, b):
        return lax.dot_general(a, b, (((0,), (0,)), ((), ())), preferred_element_type=f32)

    every = range(lots)
    tok_load.wait()
    for h in every:
        send_rows(h, jnp.dot(
            pack_own[h * rows:(h + 1) * rows, :], v_tok[...], preferred_element_type=f32
        ))

    len_col, start_col = upright_of(len_row[0:1], batch), upright_of(start_row[0:1], batch)
    count = lax.broadcasted_iota(jnp.int32, (batch, all_rows), 1).astype(f32)
    for step in range(steps):
        hit = jnp.logical_and(count == start_col + step, len_col > step)
        unpack[step * batch:(step + 1) * batch, :] = jnp.where(hit, 1.0, 0.0).astype(bf16)

    def near(gather, h):
        return (h - gather) % lots < MIXED

    def begin(h):
        x_src[h] = row_sum(h).astype(bf16)
        spread(X, h, near(0, h))
        yield
        yield from enter(0, h)

    def enter(l, h):
        k = 2 * l * lots + h
        forward(X, k, near(4 * l, h))
        yield
        weight(0, l)
        take(X, k, near(4 * l, h))
        squares = None
        for p in range(ratio):
            raw = x_recv[k, p].astype(f32)
            sq = jnp.sum(raw * raw, axis=1, keepdims=True)
            squares = sq if squares is None else squares + sq
            gain = gains[l:l + 1, pl.ds(pl.multiple_of((d * ratio + p) * cols, cols), cols)]
            norm_buf[h, :, p * cols:(p + 1) * cols] = (raw * gain).astype(bf16)
        drive = jnp.dot(norm_buf[h], v_drive[l], preferred_element_type=f32)
        high = squares.astype(bf16)
        low = (squares - high.astype(f32)).astype(bf16)
        lane = lax.broadcasted_iota(jnp.int32, (rows, width), 1)
        tail = jnp.where(
            lane == 0, high.astype(f32), jnp.where(lane == 1, low.astype(f32), 0.0)
        ).astype(bf16)
        k = l * lots + h
        for c in range(nd):
            a_send[k, c] = jnp.concatenate(
                [drive[:, c * width:(c + 1) * width].astype(bf16), tail], axis=1
            )
        trade(a_send.at[k], a_recv.at[k], a_rs.at[k], COL)
        yield
        weight(1, l)
        send_rows(
            (1 + 3 * l) * lots + h, jnp.dot(norm_buf[h], v_open[l], preferred_element_type=f32)
        )
        yield

    def recur(l):
        for h in every:
            k = l * lots + h
            summed = traded(a_send.at[k], a_recv.at[k], a_rs.at[k])
            full_sq = summed[:, width:width + 1] + summed[:, width + 1:width + 2]
            inverse = lax.rsqrt(full_sq / model + EPS)
            inv_buf[h * rows:(h + 1) * rows, :] = jnp.broadcast_to(inverse, (rows, 128))
            lane = lax.broadcasted_iota(jnp.int32, summed.shape, 1)
            feed = jnp.where(lane < width, summed * inverse, jnp.where(lane == width, 1.0, 0.0))
            feed_buf[h * rows:(h + 1) * rows, :] = feed.astype(bf16)
        arrive(st_recv.at[l], st_rs.at[l])
        real = jnp.concatenate([st_recv[l, s, 0] for s in range(nd)], axis=0)
        imag = jnp.concatenate([st_recv[l, s, 1] for s in range(nd)], axis=0)
        dr, di, gap = decays(l, 0), decays(l, 1), skips(l)
        for step in range(steps):
            span = slice(step * batch, (step + 1) * batch)
            u = jnp.dot(unpack[span, :], feed_buf[...], preferred_element_type=f32)
            live = u[:, width:width + 1] > 0.5
            push = jnp.dot(u.astype(bf16), inj[l], preferred_element_type=f32)
            moved_real = dr * real - di * imag + push[:, :own_ch]
            moved_imag = dr * imag + di * real + push[:, own_ch:]
            real = jnp.where(live, moved_real, real)
            imag = jnp.where(live, moved_imag, imag)
            both = jnp.concatenate([real, imag], axis=1).astype(bf16)
            read = lax.dot_general(
                both, omx[l], (((1,), (1,)), ((), ())), preferred_element_type=f32
            ) + gap * u
            act_buf[span, :] = jax.nn.gelu(read).astype(bf16)
        st_new[l, 0] = real
        st_new[l, 1] = imag

    def chain(l, h):
        first, second = 2 * l * lots + h, (2 * l + 1) * lots + h
        k_open = (1 + 3 * l) * lots + h
        k_merge, k_exit = k_open + lots, k_open + 2 * lots
        packed = turned(unpack[:, h * rows:(h + 1) * rows], act_buf[...]).astype(bf16)
        y_src[first] = fold(packed[:, :width])
        spread(Y, first, near(4 * l + 1, h))
        yield
        forward(Y, first, near(4 * l + 1, h))
        yield
        weight(2, l)
        wide = take_y(first, near(4 * l + 1, h))
        gating = jnp.dot(wide, v_glu[l], preferred_element_type=f32).astype(bf16)
        k = l * lots + h
        for c in range(nd):
            c_send[k, c] = fold(gating[:, c * width:(c + 1) * width])
        trade(c_send.at[k], c_recv.at[k], c_rs.at[k], COL + 1)
        yield
        summed = traded(c_send.at[k], c_recv.at[k], c_rs.at[k])
        y_src[second] = (y_src[first].astype(f32) * jax.nn.sigmoid(summed)).astype(bf16)
        spread(Y, second, near(4 * l + 2, h))
        yield
        forward(Y, second, near(4 * l + 2, h))
        yield
        weight(3, l)
        wide = take_y(second, near(4 * l + 2, h))
        send_rows(k_merge, jnp.dot(wide, v_merge[l], preferred_element_type=f32))
        yield
        mine = pl.ds(pl.multiple_of(h * rows + d * chunk, chunk), chunk)
        gate = jax.nn.sigmoid(row_sum(k_open) * inv_buf[mine, 0:1])
        x_src[second] = (gate * row_sum(k_merge)).astype(bf16)
        spread(X, second, near(4 * l + 3, h))
        yield
        forward(X, second, near(4 * l + 3, h))
        yield
        weight(4, l)
        take(X, second, near(4 * l + 3, h))
        part = None
        for p in range(ratio):
            v = jnp.dot(
                x_recv[second, p], v_exit[l, p * cols:(p + 1) * cols], preferred_element_type=f32
            )
            part = v if part is None else part + v
        send_rows(k_exit, part)
        yield
        k = (2 * l + 2) * lots + h
        x_src[k] = (x_src[first].astype(f32) + row_sum(k_exit)).astype(bf16)
        if l + 1 < layers:
            spread(X, k, near(4 * l + 4, h))
            yield
            yield from enter(l + 1, h)
        else:
            into = fin_recv.at[pl.ds(pl.multiple_of(h * rows + d * chunk, chunk), chunk)]
            pltpu.make_async_copy(x_src.at[k], into, f_rs.at[h]).start()
            for j, to in others:
                send(x_src.at[k], into, f_rs.at[h], to, t, FIN)
            yield

    def run(gather, gens, hooks):
        live, stage = set(every), 0
        while live:
            turn_of = gather + (stage + 1) // 3
            for i in every:
                h = (turn_of + i) % lots
                if h in live:
                    try:
                        next(gens[h])
                    except StopIteration:
                        live.remove(h)
            if stage in hooks:
                hooks.pop(stage)()
            stage += 1
        for rest in hooks.values():
            rest()

    run(0, [begin(h) for h in every], {0: lambda: send_states(0)})
    for l in range(layers):
        recur(l)
        hooks = {10 if l + 1 < layers else 7: functools.partial(return_states, l)}
        if l + 1 < layers:
            hooks[7] = functools.partial(send_states, l + 1)
        run(4 * l + 1, [chain(l, h) for h in every], hooks)
    for h in every:
        arrive(fin_recv.at[pl.ds(h * rows, rows)], f_rs.at[h])
    spread = turned(pack_own[...], fin_recv[...])
    keep = turned(pack_own[...], jnp.ones((all_rows, 128), bf16))[:, 0:1]
    out_tok[...] = jnp.where(keep > 0.5, spread, v_tok[...].astype(f32)).astype(bf16)
    for l in range(layers):
        arrive(out_state.at[l], n_rs.at[l])

    def sent(like, lane):
        pltpu.make_async_copy(like, like, out_sem.at[lane]).wait()

    sent(row_recv, ROW)
    sent(a_recv, COL)
    sent(c_recv, COL + 1)
    sent(st_recv.at[:, pl.ds(0, nd - 1)], ST)
    sent(st_recv.at[:, pl.ds(0, nd - 1)], ST + 1)
    sent(len_recv, LEN)
    sent(row_recv.at[pl.ds(0, lots)], FIN)
    gathers = 2 * layers
    far, near_far = (ratio - 1) * nd, (ratio - 1) * (nd - 1)
    aside_k, whole_k = gathers * MIXED, gathers * (lots - MIXED)
    sent(x_recv.at[:, 0, pl.ds(0, (nd - 1) * chunk)], XF)
    sent(y_recv.at[:, pl.ds(0, nd - 1)], YF)
    sent(x_recv.at[pl.ds(0, whole_k), pl.ds(0, ratio - 1)], XF + 2)
    sent(y_recv.at[pl.ds(0, whole_k), pl.ds(0, far)], YF + 2)
    if MIXED:
        sent(x_near.at[pl.ds(0, aside_k)], XF + 3)
        sent(y_near.at[pl.ds(0, aside_k)], YF + 3)
        sent(x_recv.at[pl.ds(0, aside_k), pl.ds(0, ratio - 1), pl.ds(0, (nd - 1) * chunk)], XF + 4)
        sent(y_recv.at[pl.ds(0, aside_k), pl.ds(0, near_far)], YF + 4)

    @pl.when(d != home)
    def _():
        sent(x_recv.at[:, 0, pl.ds(0, chunk)], XF + 1)
        sent(y_recv.at[:, pl.ds(0, 1)], YF + 1)
        if MIXED:
            sent(x_recv.at[pl.ds(0, aside_k), pl.ds(0, ratio - 1), pl.ds(0, chunk)], XF + 5)
            sent(y_recv.at[pl.ds(0, aside_k), pl.ds(0, ratio - 1)], YF + 5)


def fused_shards(
    tokens, lengths, norm_gains, drive_proj, open_proj, glu_proj, merge_proj, exit_proj,
    decay_rate, turn_rate, group_step_width, state_in, state_out, skip_gain, carried_state,
):
    f32, bf16 = jnp.float32, jnp.bfloat16
    nd, nt = lax.axis_size("dp"), lax.axis_size("tp")
    layers = norm_gains.shape[0]
    own, steps, cols = tokens.shape
    batch = own * nd
    rows = 3 * batch
    model = cols * nt
    ratio = nt // nd
    groups_own = decay_rate.shape[1]
    few = groups_own // nd
    entries = decay_rate.shape[2]
    members = state_in.shape[-1]
    width = few * members
    own_ch = few * entries
    chunk = rows // nd

    lots = LOTS
    n_row = (1 + 3 * layers) * lots
    n_col = layers * lots
    n_all = 2 * layers * lots
    lot = rows // lots
    piece = chunk // lots
    half = lot // 2
    vm = pltpu.VMEM
    dma = pltpu.SemaphoreType.DMA
    weights = (drive_proj, open_proj, glu_proj, merge_proj, exit_proj)
    scratch = [vm(w.shape, bf16) for w in weights] + [
        vm((own * steps, cols), bf16),
        vm((layers, 2, few, members, entries), f32),
        vm((layers, 2, few, members, entries), f32),
        vm((layers, 4, groups_own, entries), f32),
        vm((layers, 2 * width, 2 * own_ch), bf16),
        vm((layers, 2 * width, 2 * own_ch), bf16),
        vm((8, batch), f32),
        vm((n_row, nd, piece, cols), bf16),
        vm((n_row, nd - 1, piece, cols), bf16),
        vm((n_col, nd, lot, 2 * width), bf16),
        vm((n_col, nd - 1, lot, 2 * width), bf16),
        vm((n_col, nd, half, 2 * width), bf16),
        vm((n_col, nd - 1, half, 2 * width), bf16),
        vm((n_all + lots, piece, cols), bf16),
        vm((n_all, ratio - 1, piece, cols), bf16),
        vm((n_all, ratio, lot, cols), bf16),
        vm((n_all, half, 2 * width), bf16),
        vm((n_all, ratio - 1, half, 2 * width), bf16),
        vm((n_all, nt, half, 2 * width), bf16),
        vm((layers, nd, 2, own, own_ch), f32),
        vm((layers, 2, batch, own_ch), f32),
        vm((rows, cols), bf16),
        vm((lots, lot, ratio * cols), bf16),
        vm((rows, 128), f32),
        vm((steps * batch, 2 * width), bf16),
        vm((rows, 2 * width), bf16),
        vm((nd - 1, 8, batch), f32),
        vm((rows, own * steps), bf16),
        vm((steps * batch, rows), bf16),
        dma((5, layers)), dma((3,)),
        dma((n_row,)), dma((n_col,)), dma((n_col,)),
        dma((n_all, ratio)), dma((n_all, ratio)),
        dma((n_all, ratio - 1)), dma((n_all, ratio - 1)),
        dma((layers,)), dma((layers,)), dma((lots,)), dma((1,)), dma((LANES,)),
    ]
    inside = pl.BlockSpec(memory_space=pltpu.VMEM)
    outside = pl.BlockSpec(memory_space=pl.ANY)
    out_rows, out_state = pl.pallas_call(
        functools.partial(fused_kernel, (layers, nd, nt, rows, model, lots)),
        out_shape=(
            jax.ShapeDtypeStruct((own * steps, cols), bf16),
            jax.ShapeDtypeStruct(carried_state.shape, f32),
        ),
        in_specs=[outside] + [inside] * 5 + [outside] * 2 + [inside] + [outside] * 6,
        out_specs=(inside, outside),
        scratch_shapes=scratch,
        compiler_params=pltpu.CompilerParams(
            collective_id=0, has_side_effects=True, vmem_limit_bytes=60 * 1024 * 1024
        ),
    )(
        tokens.reshape(own * steps, cols), lengths.reshape(1, own),
        norm_gains, decay_rate, turn_rate, group_step_width,
        jnp.swapaxes(state_in, 3, 4), state_out, skip_gain, carried_state, *weights,
    )
    return out_rows.reshape(own, steps, cols), out_state


def solution(mesh):
    in_specs = (
        P("dp", None, "tp"),
        P("dp"),
        P(),
        P(None, "dp", "tp"),
        P(None, "dp", "tp"),
        P(None, "dp", "tp"),
        P(None, "dp", "tp"),
        P(None, "dp", "tp"),
        P(None, "tp", None),
        P(None, "tp", None),
        P(None, "tp"),
        P(None, None, "tp", None, None),
        P(None, None, "tp", None, None),
        P(None, "tp"),
        P(None, None, "dp", "tp"),
    )
    out_specs = (P("dp", None, "tp"), P(None, None, "dp", "tp"))
    ways, nd = mesh.shape["tp"], mesh.shape["dp"]

    def run(*args):
        groups = args[8].shape[1] // ways
        whole_groups = groups % nd == 0 and ways % nd == 0 and ways > nd > 1
        body = fused_shards if whole_groups else shards
        return jax.shard_map(body, mesh=mesh, in_specs=in_specs, out_specs=out_specs, check_vma=False)(*args)

    return run
```
